32 devices in a mesh: sp: 8 (over z, x), tp: 4 (over y, core).
Axes of the slice: x: 2, y: 2, z: 4, core: 2. Of those that a mesh axis runs over, the one named last changes fastest.
Arguments:
- residual: bfloat16 [1024, 2048], P(('sp', 'tp')), may hold values from -6 to 6
- query_rows: bfloat16 [1024, 1024], P('sp', 'tp'), may hold values from -6 to 6
- key_rows: bfloat16 [1024, 512], P('sp', 'tp'), may hold values from -6 to 6
- value_rows: bfloat16 [1024, 512], P('sp', 'tp'), may hold values from -8 to 8
- head_offset: float32 [8], P('tp'), may hold values from -13 to -3
- w_out: bfloat16 [1024, 2048], P('tp'), may hold values from -0.5 to 0.5
- norm_gain: float32 [2, 2048], replicated, may hold values from 0.1 to 1.9
- norm_bias: float32 [2, 2048], replicated, may hold values from -1.5 to 1.5
- routing: int32 [1024, 2], P(('sp', 'tp')), may hold values from 0 to 7, all different within a row; in each aligned block of 32 rows (0 to 31, 32 to 63, ...) at most 12 rows name the same one
- route_weight: float32 [1024, 2], P(('sp', 'tp')), may hold values from 0.2 to 1
- w_exp_gate: bfloat16 [8, 2048, 1024], P('sp', None, 'tp'), may hold values from -0.125 to 0.125
- w_exp_up: bfloat16 [8, 2048, 1024], P('sp', None, 'tp'), may hold values from -0.125 to 0.125
- w_exp_down: bfloat16 [8, 1024, 2048], P('sp', 'tp'), may hold values from -0.1875 to 0.1875
- w_shared_gate: bfloat16 [2048, 1024], P(None, 'tp'), may hold values from -0.125 to 0.125
- w_shared_up: bfloat16 [2048, 1024], P(None, 'tp'), may hold values from -0.125 to 0.125
- w_shared_down: bfloat16 [1024, 2048], P('tp'), may hold values from -0.1875 to 0.1875
Outputs:
- result: bfloat16 [1024, 2048], P(('sp', 'tp'))
The draws below stay inside these ranges and needn't reach their ends.
Inputs may be any that keep to these rules, and one draw needn't show every extreme that they name: `routing`: each row names 2 different experts; within the rows of one device (32 tokens) no expert is named by more than 12 of them, a bound that some block reaches.
All inputs are finite; a program needn't handle non-finite values.
Results may differ from the reference program's by a relative error of at most 0.013.
Values may be sent and summed in bfloat16 or wider, within the bound.
A program may use at most 64 MiB of HBM per device.

```python
import math
import jax
import jax.numpy as jnp
import numpy as np
from jax import lax

D = 2048
HEADS = 8
DH = 128
KV_HEADS = 4
EXPERT_FF = 1024
SHARED_FF = 1024
TOP_K = 2
TOK_DEV = 128
TOKENS = 1024
ROWS_DEV = 32
EXPERTS = 8
CAP = 12
N_TP = 4


def draw_value_rows(key, part):
    key_center = jax.random.fold_in(key, 11)
    key_noise = jax.random.fold_in(key, 12)
    center = jnp.clip(jax.random.normal(key_center, (1, KV_HEADS * DH), jnp.float32), -1.0, 1.0)
    noise = 2.0 * jnp.clip(jax.random.normal(key_noise, (TOKENS, KV_HEADS * DH), jnp.float32), -3.5, 3.5)
    return (center + noise).astype(jnp.bfloat16)


def draw_head_offset(key, part):
    key_pick = jax.random.fold_in(key, 21)
    key_slow = jax.random.fold_in(key, 22)
    key_fast = jax.random.fold_in(key, 23)
    keep_share = 0.5
    slow_heads = jax.random.uniform(key_pick, (HEADS,), jnp.float32) < keep_share
    slow_value = -jnp.log(0.6 * TOKENS) + jax.random.uniform(key_slow, (HEADS,), jnp.float32, -0.5, 0.5)
    fast_value = -jax.random.uniform(key_fast, (HEADS,), jnp.float32, 3.0, 4.5)
    return jnp.where(slow_heads, slow_value, fast_value).astype(jnp.float32)


def steps_of(rng, dims, cuts, smallest, high):
    def one(axis_at, blocks):
        draws = jax.random.uniform(jax.random.fold_in(jax.random.fold_in(rng, 6), axis_at), (blocks,), jnp.float32, smallest / len(cuts), high / len(cuts))
        return jnp.repeat(jnp.exp(draws), dims[axis_at] // blocks).reshape((-1,) + (1,) * (len(dims) - axis_at - 1))

    level = one(*cuts[0])
    for cut in cuts[1:]:
        level = level * one(*cut)
    return level


def routed_block(stream_key, own, number, rows, amount, top, reach, lean):
    sequence = jax.random.permutation(stream_key, amount)
    crowded, usual = shares(amount, rows * top, reach, lean, True), shares(amount, rows * top, reach, lean, False)
    places = jnp.arange(amount)

    def named(lengths, rotation):
        used = int((lengths > 0).sum())
        fixed = max(1, used // 4)
        moved = fixed + (places - fixed + rotation * (used - fixed)) % max(1, amount - fixed)
        return jnp.zeros((amount,), jnp.int32).at[sequence[jnp.where(places < fixed, places, moved)]].set(jnp.asarray(lengths, jnp.int32))

    lengths = jnp.where(number % 4 == 0, named(crowded, number // 4), named(usual, number - number // 4 - 1))
    mixed = jax.random.permutation(jax.random.fold_in(own, 3), amount)
    donor, sink = mixed[0:amount // 2 * 2:2], mixed[1:amount // 2 * 2:2]
    room = jnp.minimum(lengths[donor] - 1, reach - lengths[sink]) // 2
    room = jnp.where((donor == sequence[0]) | (sink == sequence[0]) | (lengths[sink] == 0), 0, jnp.maximum(room, 0))
    moved = jax.random.randint(jax.random.fold_in(own, 4), (amount // 2,), 0, 1 << 20) % (room + 1)
    lengths = lengths.at[donor].add(-moved).at[sink].add(moved)
    members = jnp.searchsorted(jnp.cumsum(lengths), jnp.arange(rows * top), side="right").astype(jnp.int32)
    listing = members.reshape(top, rows).T
    listing = listing[jax.random.permutation(jax.random.fold_in(own, 1), rows)]
    rotation = jax.random.randint(jax.random.fold_in(own, 2), (rows, 1), 0, top)
    return jnp.take_along_axis(listing, (jnp.arange(top)[None, :] + rotation) % top, axis=1)


def shares(amount, total, limit, skew, full):
    weights = [(1 << 20) // math.isqrt(standing ** skew) + 1 for standing in range(1, amount + 1)]
    largest = limit if full else min(limit, max(-(-total // amount), total * weights[0] // sum(weights)))
    least = 1 if total - largest >= amount - 1 else 0
    given, spare = [largest] + [least] * (amount - 1), total - largest - least * (amount - 1)
    while spare > 0:
        free = [i for i in range(1, amount) if given[i] < largest] or [i for i in range(1, amount) if given[i] < limit]
        pool, left = sum([weights[i] for i in free]), spare
        for i in free:
            more = min(limit - given[i], max(1, left * weights[i] // pool), spare)
            given[i] = given[i] + more
            spare = spare - more
    return np.array(given)


def centred(own_key, dims, deviation, reach, pieces=(), held_as=jnp.bfloat16):
    level = steps_of(own_key, dims, pieces, -0.22, 0.18) if pieces else 1.0
    array = jax.random.normal(own_key, dims, jnp.float32) * deviation * level
    return jnp.minimum(jnp.maximum(array, -reach), reach).astype(held_as)


def setup_inputs(seed: int = 0) -> dict:
    streams_of = jax.random.split(jax.random.key(seed), 17)
    residual = centred(streams_of[0], (TOKENS, D), 1.0, 6.0, ((0, 32),))
    query_rows = centred(streams_of[1], (TOKENS, HEADS * DH), 1.0, 6.0, ((0, 8), (1, 4)))
    key_rows = centred(streams_of[2], (TOKENS, KV_HEADS * DH), 1.0, 6.0, ((0, 8), (1, 4)))
    value_rows = draw_value_rows(jax.random.fold_in(streams_of[16], 71), 0)
    head_offset = draw_head_offset(jax.random.fold_in(streams_of[16], 71), 0)
    w_out = centred(streams_of[5], (HEADS * DH, D), (HEADS * DH // 8) ** -0.5, 0.5, ((0, 4),))
    norm_gain = jnp.clip(1.0 + 0.18 * jax.random.normal(streams_of[6], (2, D), jnp.float32), 0.1, 1.9)
    norm_bias = centred(streams_of[7], (2, D), 0.3, 1.5, (), jnp.float32)
    routing_keys = jax.random.split(jax.random.fold_in(streams_of[8], 1), TOKENS // ROWS_DEV)
    routing_turns = jax.random.permutation(jax.random.fold_in(streams_of[8], 3), TOKENS // ROWS_DEV)
    routing = jax.vmap(lambda own, number: routed_block(jax.random.fold_in(streams_of[8], 2), own, number, ROWS_DEV, EXPERTS, TOP_K, CAP, 1))(routing_keys, routing_turns).reshape((TOKENS, TOP_K))
    route_weight = jnp.clip(0.2 + 0.8 * jax.random.uniform(streams_of[9], (TOKENS, TOP_K), jnp.float32) ** steps_of(streams_of[9], (TOKENS, TOP_K), ((0, 32),), -0.2, 0.2), 0.2, 1.0)
    w_exp_gate = centred(streams_of[10], (EXPERTS, D, EXPERT_FF), D ** -0.5, 0.125, ((0, 8), (2, 4)))
    w_exp_up = centred(streams_of[11], (EXPERTS, D, EXPERT_FF), D ** -0.5, 0.125, ((0, 8), (2, 4)))
    w_exp_down = centred(streams_of[12], (EXPERTS, EXPERT_FF, D), EXPERT_FF ** -0.5, 0.1875, ((0, 8), (1, 4)))
    w_shared_gate = centred(streams_of[13], (D, SHARED_FF), D ** -0.5, 0.125, ((1, 4),))
    w_shared_up = centred(streams_of[14], (D, SHARED_FF), D ** -0.5, 0.125, ((1, 4),))
    w_shared_down = centred(streams_of[15], (SHARED_FF, D), SHARED_FF ** -0.5, 0.1875, ((0, 4),))
    return dict(residual=residual, query_rows=query_rows, key_rows=key_rows, value_rows=value_rows, head_offset=head_offset, w_out=w_out, norm_gain=norm_gain, norm_bias=norm_bias, routing=routing, route_weight=route_weight, w_exp_gate=w_exp_gate, w_exp_up=w_exp_up, w_exp_down=w_exp_down, w_shared_gate=w_shared_gate, w_shared_up=w_shared_up, w_shared_down=w_shared_down)


ALPHA = 8.0 ** 0.25
LN_EPS = 1e-05

def layer_norm(summed, gain, shift):
    center = summed - lax.optimization_barrier(jnp.mean(summed, axis=-1, keepdims=True))
    spread = lax.optimization_barrier(jnp.mean(center * center, axis=-1, keepdims=True))
    return (center * lax.rsqrt(spread + LN_EPS) * gain + shift).astype(jnp.bfloat16)

def split_down(hidden, down_weight, group_len):
    total = jnp.zeros((hidden.shape[0], down_weight.shape[1]), jnp.float32)
    for group_index in range(N_TP):
        lower = group_index * group_len
        part = jnp.dot(hidden[:, lower:lower + group_len], down_weight[lower:lower + group_len], preferred_element_type=jnp.float32)
        rounded = lax.optimization_barrier(part.astype(jnp.bfloat16))
        total = total + rounded.astype(jnp.float32)
    return total.astype(jnp.bfloat16)

def reference(residual, query_rows, key_rows, value_rows, head_offset, w_out, norm_gain, norm_bias, routing, route_weight, w_exp_gate, w_exp_up, w_exp_down, w_shared_gate, w_shared_up, w_shared_down):
    group_size = HEADS // KV_HEADS
    queries = query_rows.astype(jnp.float32).reshape(TOKENS, KV_HEADS, group_size, DH)
    keys_all = key_rows.astype(jnp.float32).reshape(TOKENS, KV_HEADS, DH)
    values_all = value_rows.astype(jnp.float32).reshape(TOKENS, KV_HEADS, DH)
    offset = head_offset.reshape(KV_HEADS, group_size)
    key_pos = jnp.arange(TOKENS, dtype=jnp.int32)

    def attend_block(first_row):
        block_queries = lax.dynamic_slice_in_dim(queries, first_row, TOK_DEV, 0)
        scores = jnp.einsum('tkgd,skd->kgts', block_queries, keys_all)
        scores = scores * DH ** (-0.5) + offset[:, :, None, None]
        query_pos = (first_row + jnp.arange(TOK_DEV, dtype=jnp.int32)).astype(jnp.int32)
        causal = key_pos[None, :] < query_pos[:, None]
        leftover = jnp.where(causal, jax.nn.log_sigmoid(-scores), 0.0)
        passed = lax.cumsum(leftover, axis=3, reverse=True) - leftover
        weights = jnp.where(causal, jnp.exp(jax.nn.log_sigmoid(scores) + passed), 0.0).astype(jnp.bfloat16)
        output = jnp.einsum('kgts,skd->tkgd', weights.astype(jnp.float32), values_all)
        return output.astype(jnp.bfloat16)
    starts = (jnp.arange(TOKENS // TOK_DEV, dtype=jnp.int32) * TOK_DEV).astype(jnp.int32)
    attended = lax.map(attend_block, starts).reshape(TOKENS, HEADS * DH)
    group_rows = HEADS * DH // N_TP
    mixed = jnp.zeros((TOKENS, D), jnp.float32)
    for group_index in range(N_TP):
        lower = group_index * group_rows
        part = jnp.dot(attended[:, lower:lower + group_rows], w_out[lower:lower + group_rows], preferred_element_type=jnp.float32)
        rounded = lax.optimization_barrier(part.astype(jnp.bfloat16))
        mixed = mixed + rounded.astype(jnp.float32)
    normed = layer_norm(ALPHA * residual.astype(jnp.float32) + mixed, norm_gain[0], norm_bias[0])
    blocks = TOKENS // ROWS_DEV
    flat_routes = routing.reshape(blocks, ROWS_DEV * TOP_K)
    one_hot = (flat_routes[..., None] == jnp.arange(EXPERTS, dtype=jnp.int32)[None, None, :]).astype(jnp.int32)
    slot_rank = lax.optimization_barrier(jnp.sum((jnp.cumsum(one_hot, axis=1) - 1) * one_hot, axis=2))
    token_of = (jnp.arange(blocks, dtype=jnp.int32)[:, None] * ROWS_DEV + jnp.arange(ROWS_DEV * TOP_K, dtype=jnp.int32)[None, :] // TOP_K).astype(jnp.int32)
    block_ids = jnp.broadcast_to(jnp.arange(blocks, dtype=jnp.int32)[:, None], flat_routes.shape)
    table = jnp.full((blocks, EXPERTS * CAP), TOKENS, jnp.int32).at[block_ids, flat_routes * CAP + slot_rank].set(token_of)
    table = table.reshape(blocks, EXPERTS, CAP).transpose(1, 0, 2).reshape(EXPERTS, blocks * CAP)
    ff_group = EXPERT_FF // N_TP

    def run_expert(packed):
        index_rows, gate_weight, up_weight, down_weight = packed
        rows = jnp.take(normed, index_rows, axis=0, mode='fill', fill_value=0)
        gate_part = jnp.dot(rows, gate_weight, preferred_element_type=jnp.float32)
        up_part = jnp.dot(rows, up_weight, preferred_element_type=jnp.float32)
        hidden = (jax.nn.silu(gate_part) * up_part).astype(jnp.bfloat16)
        return split_down(hidden, down_weight, ff_group)
    expert_outs = lax.map(run_expert, (table, w_exp_gate, w_exp_up, w_exp_down))
    place = (block_ids * CAP + slot_rank).astype(jnp.int32)
    picked = expert_outs[flat_routes, place].reshape(TOKENS, TOP_K, D).astype(jnp.float32)
    routed = lax.optimization_barrier(jnp.sum(picked * route_weight[:, :, None], axis=1))
    shared_gate = jnp.dot(normed, w_shared_gate, preferred_element_type=jnp.float32)
    shared_up = jnp.dot(normed, w_shared_up, preferred_element_type=jnp.float32)
    shared_hidden = (jax.nn.silu(shared_gate) * shared_up).astype(jnp.bfloat16)
    shared_out = lax.optimization_barrier(split_down(shared_hidden, w_shared_down, SHARED_FF // N_TP))
    combined = routed + shared_out.astype(jnp.float32)
    return layer_norm(ALPHA * normed.astype(jnp.float32) + combined, norm_gain[1], norm_bias[1])
```

```python
import functools

import jax
import jax.numpy as jnp
from jax import lax
from jax.experimental import pallas as pl
from jax.experimental.pallas import tpu as pltpu
from jax.sharding import PartitionSpec as P

DH = 128
ALPHA = 8.0**0.25
LN_EPS = 1e-05
BF = jnp.bfloat16
F32 = jnp.float32
MESH = pl.DeviceIdType.MESH


def dot(a, b):
    return jnp.dot(a, b, preferred_element_type=F32)


def silu_mul(g, u):
    return (g / (1.0 + jnp.exp(-g)) * u).astype(BF)


def layer_norm(x0, x1, gain, bias):
    width = x0.shape[1]
    total = 2 * width
    mean = (jnp.sum(x0, axis=1, keepdims=True) + jnp.sum(x1, axis=1, keepdims=True)) / total
    x0, x1 = x0 - mean, x1 - mean
    spread = (
        jnp.sum(x0 * x0, axis=1, keepdims=True) + jnp.sum(x1 * x1, axis=1, keepdims=True)
    ) / total
    inv = lax.rsqrt(spread + LN_EPS)
    n0 = (x0 * inv * gain[:, :width] + bias[:, :width]).astype(BF)
    n1 = (x1 * inv * gain[:, width:] + bias[:, width:]).astype(BF)
    return n0, n1


def kernel(
    cfg, res, q, k, v, off, wout, gain, bias, routing, rw, wg, wu, wd, sg, su, sd, out,
    wout_v, wg_v, wu_v, wd_v, sg_v, su_v, sd_v,
    kbuf, vbuf, acc, beyond, pj, r1, ys1, yr1, mixh, resall, rall, rwall,
    tok, outg, xb, yb, rb, ry, zb, ret, spart, rs, rsy, fin,
    wsem, ksend, krecv, vsend, vrecv, dsend, drecv, ysend, yrecv, asend, arecv,
    bsend, brecv, y3send, y3recv, zsend, zrecv, msend, mrecv,
):
    n, cap2, rows = cfg
    i, t = lax.axis_index("sp"), lax.axis_index("tp")
    c, y = lax.rem(t, 2), lax.div(t, 2)
    oc, oy = 1 - c, 1 - y
    mate, across = t + 1 - 2 * c, t + 2 - 4 * y
    shard = q.shape[0]
    half = out.shape[1] // 2
    pair = 2 * rows

    weights = [
        pltpu.make_async_copy(src, dst, wsem.at[a])
        for a, (src, dst) in enumerate(
            [(wout, wout_v), (sg, sg_v), (su, su_v), (sd, sd_v),
             (wg.at[0], wg_v), (wu.at[0], wu_v), (wd.at[0], wd_v)]
        )
    ]
    for cp in weights:
        cp.start()

    barrier = pltpu.get_barrier_semaphore()

    def hello(d, _):
        pl.semaphore_signal(
            barrier, inc=1, device_id={"sp": lax.rem(i + d, n), "tp": t}, device_id_type=MESH
        )
        return 0

    lax.fori_loop(1, n, hello, 0)
    for peer in (mate, across):
        pl.semaphore_signal(barrier, inc=1, device_id={"sp": i, "tp": peer}, device_id_type=MESH)
    pl.semaphore_wait(barrier, n + 1)

    def rcopy(src, dst, ssem, rsem, sp, tp):
        return pltpu.make_async_remote_copy(
            src_ref=src, dst_ref=dst, send_sem=ssem, recv_sem=rsem,
            device_id={"sp": sp, "tp": tp}, device_id_type=MESH,
        )

    def small(m, src, dst, peer):
        return rcopy(src, dst, msend.at[m], mrecv.at[m], i, peer)

    def kcopy(dest, slot):
        return rcopy(k, kbuf.at[slot], ksend.at[dest], krecv.at[slot], dest, t)

    def vcopy(dest, slot):
        return rcopy(v, vbuf.at[slot], vsend.at[dest], vrecv.at[slot], dest, t)

    def push(d, _):
        kcopy(i + d, i).start()
        vcopy(i + d, i).start()
        return 0

    lax.fori_loop(1, n - i, push, 0)
    m_res = small(0, res, resall.at[c], mate)
    m_rou = small(1, routing, rall.at[c], mate)
    m_rw = small(2, rw, rwall.at[c], mate)
    for cp in (m_res, m_rou, m_rw):
        cp.start()
    resall[c] = res[...]
    rall[c] = routing[...]
    rwall[c] = rw[...]

    heads = q.shape[1] // DH
    hq = heads * shard
    q2 = jnp.concatenate([q[:, h * DH:(h + 1) * DH] for h in range(heads)], axis=0)
    row = lax.broadcasted_iota(jnp.int32, (hq, shard), 0)
    col = lax.broadcasted_iota(jnp.int32, (hq, shard), 1)
    offs = jnp.full((hq, shard), off[0], F32)
    for h in range(1, heads):
        offs = jnp.where(row >= h * shard, off[h], offs)
    trow = lax.broadcasted_iota(jnp.int32, (shard, shard), 0)
    tcol = lax.broadcasted_iota(jnp.int32, (shard, shard), 1)
    later = jnp.where(trow > tcol, 1.0, 0.0).astype(BF)
    scale = DH**-0.5

    def stick(kb, vb, causal, prior):
        s = lax.dot_general(q2, kb, (((1,), (1,)), ((), ())), preferred_element_type=F32)
        s = s * scale + offs
        soft = jnp.maximum(s, 0.0) + jnp.log(1.0 + jnp.exp(-jnp.abs(s)))
        left = -soft if causal is None else jnp.where(causal, -soft, 0.0)
        hi = left.astype(BF)
        lo = (left - hi.astype(F32)).astype(BF)
        within = dot(hi, later) + dot(lo, later)
        w = jnp.exp(s - soft + within + prior)
        if causal is not None:
            w = jnp.where(causal, w, 0.0)
        total = jnp.sum(left, axis=1, keepdims=True)
        return dot(w.astype(BF), vb), total

    o, total = stick(k[...], v[...], col < lax.rem(row, shard), 0.0)
    acc[...] = o
    beyond[...] = jnp.broadcast_to(total, (hq, shard))

    def block(d, _):
        src = i - d
        kcopy(i, src).wait_recv()
        vcopy(i, src).wait_recv()
        o, total = stick(kbuf[src], vbuf[src], None, beyond[...])
        acc[...] += o
        beyond[...] += total
        return 0

    lax.fori_loop(1, i + 1, block, 0)
    att = jnp.concatenate(
        [acc[h * shard:(h + 1) * shard, :] for h in range(heads)], axis=1
    ).astype(BF)

    weights[0].wait()

    def project(h):
        columns = pl.ds(pl.multiple_of(h * half, half), half)
        pj[h] = dot(att, wout_v[:, columns]).astype(BF)

    project(oc)
    m_pj = small(3, pj.at[oc], r1, mate)
    m_pj.start()
    project(c)
    m_pj.wait_recv()
    mine_rows = pl.ds(pl.multiple_of(y * pair, pair), pair)
    other_rows = pl.ds(pl.multiple_of(oy * pair, pair), pair)
    ys1[...] = (pj[c, other_rows, :].astype(F32) + r1[other_rows, :].astype(F32)).astype(BF)
    m_y1 = small(4, ys1, yr1, across)
    m_y1.start()

    m_rou.wait_recv()
    m_rw.wait_recv()
    width = n * cap2
    rt = jnp.concatenate([rall[0], rall[1]], axis=0)
    rt0, rt1 = rt[:, 0:1], rt[:, 1:2]
    wt = jnp.concatenate([rwall[0], rwall[1]], axis=0)
    wcol = lax.broadcasted_iota(jnp.int32, (pair, width), 1)
    e_of = lax.div(wcol, cap2)
    r_of = wcol - e_of * cap2
    is0, is1 = rt0 == e_of, rt1 == e_of
    named = jnp.where(is0 | is1, 1.0, 0.0)
    before = jnp.where(
        lax.broadcasted_iota(jnp.int32, (pair, pair), 0)
        > lax.broadcasted_iota(jnp.int32, (pair, pair), 1), 1.0, 0.0
    ).astype(BF)
    rank = dot(before, named.astype(BF))
    place = jnp.where(rank == r_of.astype(F32), named, 0.0)
    back = place * jnp.where(is0, wt[:, 0:1], wt[:, 1:2])
    place_t = place.T.astype(BF)

    m_y1.wait_recv()
    mixh[c] = (
        pj[c, mine_rows, :].astype(F32) + r1[mine_rows, :].astype(F32) + yr1[...].astype(F32)
    )
    m_mix = small(5, mixh.at[c], mixh.at[c], mate)
    m_mix.start()
    m_res.wait_recv()
    small(5, mixh.at[oc], mixh.at[oc], mate).wait_recv()
    resid = jnp.concatenate([resall[0], resall[1]], axis=0)
    n0, n1 = layer_norm(
        ALPHA * resid[:, :half].astype(F32) + mixh[0],
        ALPHA * resid[:, half:].astype(F32) + mixh[1],
        gain[0:1, :], bias[0:1, :],
    )
    tok[y, 0] = n0
    tok[y, 1] = n1
    m_tok = small(6, tok.at[y, c], tok.at[y, c], across)
    m_tok.start()

    chosen = dot(place_t, tok[y, c])
    for e in range(n):
        outg[e] = chosen[e * cap2:(e + 1) * cap2, :].astype(BF)

    def dcopy(dest, slot):
        return rcopy(
            outg.at[dest], xb.at[c, y, slot], dsend.at[dest], drecv.at[slot], dest, t
        )

    def send_out(d, _):
        dcopy(lax.rem(i + d, n), i).start()
        return 0

    lax.fori_loop(1, n, send_out, 0)
    xb[c, y, i] = outg[i]

    def ycopy(slot, yy):
        ref = xb.at[c, yy, slot]
        return rcopy(ref, ref, ysend.at[slot], yrecv.at[slot], i, across)

    def acopy(slot, cc):
        ref = xb.at[cc, y, slot]
        return rcopy(ref, ref, asend.at[slot], arecv.at[slot], i, mate)

    def bcopy(slot, cc):
        ref = xb.at[cc, oy, slot]
        return rcopy(ref, ref, bsend.at[slot], brecv.at[slot], i, mate)

    def forward(slot):
        ycopy(slot, y).start()
        acopy(slot, c).start()

    forward(i)
    small(6, tok.at[oy, c], tok.at[oy, c], across).wait_recv()
    m_tok2 = small(7, tok.at[oy, c], tok.at[oy, c], mate)
    m_tok2.start()

    def relay(d, _):
        src = lax.rem(i + n - d, n)
        dcopy(i, src).wait_recv()
        forward(src)
        return 0

    lax.fori_loop(1, n, relay, 0)

    small(7, tok.at[oy, oc], tok.at[oy, oc], mate).wait_recv()
    for cp in weights[1:4]:
        cp.wait()
    t0 = jnp.concatenate([tok[0, 0], tok[1, 0]], axis=0)
    t1 = jnp.concatenate([tok[0, 1], tok[1, 1]], axis=0)
    gate = dot(t0, sg_v[:half, :]) + dot(t1, sg_v[half:, :])
    up = dot(t0, su_v[:half, :]) + dot(t1, su_v[half:, :])
    hid = silu_mul(gate, up)
    for h in range(2):
        spart[h] = dot(hid, sd_v[:, h * half:(h + 1) * half]).astype(BF)
    m_sp = small(8, spart.at[oc], rs, mate)
    m_sp.start()

    def relay2(d, _):
        src = lax.rem(i + n - d, n)
        ycopy(src, oy).wait_recv()
        bcopy(src, c).start()
        return 0

    lax.fori_loop(0, n, relay2, 0)
    m_sp.wait_recv()
    ys1s = (spart[c, other_rows, :].astype(F32) + rs[other_rows, :].astype(F32)).astype(BF)
    spart[c, other_rows, :] = ys1s
    m_sy = small(9, spart.at[c, other_rows, :], rsy, across)
    m_sy.start()

    def gathered(d, _):
        src = lax.rem(i + n - d, n)
        acopy(src, oc).wait_recv()
        bcopy(src, oc).wait_recv()
        return 0

    lax.fori_loop(0, n, gathered, 0)
    for cp in weights[4:]:
        cp.wait()
    count = 2 * n * cap2
    hidden = []
    for yy in range(2):
        x0 = xb[0, yy].astype(F32).reshape(n * cap2, half).astype(BF)
        x1 = xb[1, yy].astype(F32).reshape(n * cap2, half).astype(BF)
        gate = dot(x0, wg_v[:half, :]) + dot(x1, wg_v[half:, :])
        up = dot(x0, wu_v[:half, :]) + dot(x1, wu_v[half:, :])
        hidden.append(silu_mul(gate, up))
    hid = jnp.concatenate(hidden, axis=0)

    def down(h):
        columns = pl.ds(pl.multiple_of(h * half, half), half)
        part = dot(hid, wd_v[:, columns]).reshape(2, n, cap2, half)
        yb[h] = part.astype(BF)

    down(oc)
    m_yb0 = small(10, yb.at[oc, oy], rb.at[oy], mate)
    m_yb1 = small(11, yb.at[oc, y], rb.at[y], mate)
    m_yb0.start()
    m_yb1.start()
    down(c)

    def y3copy(slot):
        return rcopy(
            yb.at[c, oy, slot], ry.at[slot], y3send.at[slot], y3recv.at[slot], i, across
        )

    def zcopy(dest, slot):
        return rcopy(zb.at[dest], ret.at[slot], zsend.at[dest], zrecv.at[slot], dest, t)

    small(10, yb.at[oc, oy], rb.at[oy], mate).wait_recv()

    def fold(d, _):
        j = lax.rem(i + d, n)
        yb[c, oy, j] = (yb[c, oy, j].astype(F32) + rb[oy, j].astype(F32)).astype(BF)
        y3copy(j).start()
        return 0

    lax.fori_loop(1, n + 1, fold, 0)
    small(11, yb.at[oc, y], rb.at[y], mate).wait_recv()

    def fold2(d, _):
        j = lax.rem(i + d, n)
        y3copy(j).wait_recv()
        zb[j] = (
            yb[c, y, j].astype(F32) + rb[y, j].astype(F32) + ry[j].astype(F32)
        ).astype(BF)
        zcopy(j, i).start()
        return 0

    lax.fori_loop(1, n, fold2, 0)
    y3copy(i).wait_recv()
    ret[i] = (yb[c, y, i].astype(F32) + rb[y, i].astype(F32) + ry[i].astype(F32)).astype(BF)

    m_sy.wait_recv()
    shared = (
        spart[c, mine_rows, :].astype(F32) + rs[mine_rows, :].astype(F32) + rsy[...].astype(F32)
    ).astype(BF).astype(F32)
    b_hi = back.astype(BF)
    b_lo = (back - b_hi.astype(F32)).astype(BF)

    def returned(d, _):
        zcopy(i, lax.rem(i + n - d, n)).wait_recv()
        return 0

    lax.fori_loop(1, n, returned, 0)
    rows_back = ret[...].astype(F32).reshape(width, half).astype(BF)
    m_mix.wait_send()
    mixh[0] = shared + dot(b_hi, rows_back) + dot(b_lo, rows_back)
    own = pl.ds(pl.multiple_of(c * rows, rows), rows)
    theirs = pl.ds(pl.multiple_of(oc * rows, rows), rows)
    fin[2] = mixh[0, theirs, :]
    fin[c] = mixh[0, own, :]
    m_fin = small(12, fin.at[2], fin.at[c], mate)
    m_fin.start()
    small(12, fin.at[2], fin.at[oc], mate).wait_recv()
    n0, n1 = layer_norm(
        ALPHA * tok[y, 0, own, :].astype(F32) + fin[0],
        ALPHA * tok[y, 1, own, :].astype(F32) + fin[1],
        gain[1:2, :], bias[1:2, :],
    )
    out[:, :half] = n0
    out[:, half:] = n1

    def sent_kv(d, _):
        kcopy(i + d, i).wait_send()
        vcopy(i + d, i).wait_send()
        return 0

    lax.fori_loop(1, n - i, sent_kv, 0)

    def sent(d, _):
        j = lax.rem(i + d, n)
        dcopy(j, i).wait_send()
        zcopy(j, i).wait_send()
        return 0

    lax.fori_loop(1, n, sent, 0)

    def sent_all(j, _):
        ycopy(j, y).wait_send()
        acopy(j, c).wait_send()
        bcopy(j, c).wait_send()
        y3copy(j).wait_send()
        return 0

    lax.fori_loop(0, n, sent_all, 0)
    for cp in (m_res, m_rou, m_rw, m_pj, m_y1, m_tok, m_tok2, m_sp, m_sy, m_yb0, m_yb1, m_fin):
        cp.wait_send()


def per_device(
    residual, query_rows, key_rows, value_rows, head_offset, w_out, norm_gain, norm_bias,
    routing, route_weight, w_exp_gate, w_exp_up, w_exp_down, w_shared_gate, w_shared_up,
    w_shared_down,
):
    n = lax.axis_size("sp")
    rows, width = residual.shape
    shard = query_rows.shape[0]
    half = width // 2
    heads = query_rows.shape[1] // DH
    ff = w_exp_gate.shape[2]
    sff = w_shared_gate.shape[1]
    pair = 2 * rows
    experts = n * w_exp_gate.shape[0]
    assert w_exp_gate.shape[0] == 1 and key_rows.shape[1] == DH and lax.axis_size("tp") == 4
    cap = max(2, 3 * rows * routing.shape[1] // (2 * experts))
    cap2 = -(-2 * cap // 8) * 8
    vm = pl.BlockSpec(memory_space=pltpu.VMEM)
    anyw = pl.BlockSpec(memory_space=pl.ANY)
    smem = pl.BlockSpec(memory_space=pltpu.SMEM)
    dma = pltpu.SemaphoreType.DMA
    V = pltpu.VMEM
    scratch = [
        V(w_out.shape, BF), V(w_exp_gate.shape[1:], BF), V(w_exp_up.shape[1:], BF),
        V(w_exp_down.shape[1:], BF), V(w_shared_gate.shape, BF), V(w_shared_up.shape, BF),
        V(w_shared_down.shape, BF),
        V((n, shard, DH), BF), V((n, shard, DH), BF),
        V((heads * shard, DH), F32), V((heads * shard, shard), F32),
        V((2, shard, half), BF), V((shard, half), BF),
        V((pair, half), BF), V((pair, half), BF),
        V((2, pair, half), F32), V((2, rows, width), BF),
        V((2,) + routing.shape, jnp.int32), V((2,) + route_weight.shape, F32),
        V((2, 2, pair, half), BF),
        V((n, cap2, half), BF),
        V((2, 2, n, cap2, half), BF),
        V((2, 2, n, cap2, half), BF),
        V((2, n, cap2, half), BF),
        V((n, cap2, half), BF), V((n, cap2, half), BF), V((n, cap2, half), BF),
        V((2, shard, half), BF), V((shard, half), BF), V((pair, half), BF),
        V((3, rows, half), F32),
        dma((7,)),
    ] + [dma((n,))] * 16 + [dma((13,)), dma((13,))]
    return pl.pallas_call(
        functools.partial(kernel, (n, cap2, rows)),
        out_shape=jax.ShapeDtypeStruct(residual.shape, BF),
        in_specs=[vm, vm, vm, vm, smem, anyw, vm, vm, vm, vm] + [anyw] * 6,
        out_specs=vm,
        scratch_shapes=scratch,
        compiler_params=pltpu.CompilerParams(
            collective_id=0, has_side_effects=True, vmem_limit_bytes=56 * 1024 * 1024
        ),
    )(
        residual, query_rows, key_rows, value_rows, head_offset, w_out, norm_gain, norm_bias,
        routing, route_weight, w_exp_gate, w_exp_up, w_exp_down, w_shared_gate, w_shared_up,
        w_shared_down,
    )


def solution(mesh):
    placed = (
        P(("sp", "tp"), None),
        P("sp", "tp"),
        P("sp", "tp"),
        P("sp", "tp"),
        P("tp"),
        P("tp", None),
        P(),
        P(),
        P(("sp", "tp"), None),
        P(("sp", "tp"), None),
        P("sp", None, "tp"),
        P("sp", None, "tp"),
        P("sp", "tp", None),
        P(None, "tp"),
        P(None, "tp"),
        P("tp", None),
    )
    return jax.shard_map(
        per_device, mesh=mesh, in_specs=placed, out_specs=P(("sp", "tp"), None), check_vma=False
    )
```

```python
import functools

import jax
import jax.numpy as jnp
from jax import lax
from jax.experimental import pallas as pl
from jax.experimental.pallas import tpu as pltpu
from jax.sharding import PartitionSpec as P

DH = 128
ALPHA = 8.0**0.25
LN_EPS = 1e-05
BF = jnp.bfloat16
F32 = jnp.float32
MESH = pl.DeviceIdType.MESH


def dot(a, b):
    return jnp.dot(a, b, preferred_element_type=F32)


def silu_mul(g, u):
    return (g / (1.0 + jnp.exp(-g)) * u).astype(BF)


def layer_norm(x0, x1, gain, bias):
    width = x0.shape[1]
    total = 2 * width
    mean = (jnp.sum(x0, axis=1, keepdims=True) + jnp.sum(x1, axis=1, keepdims=True)) / total
    x0, x1 = x0 - mean, x1 - mean
    spread = (
        jnp.sum(x0 * x0, axis=1, keepdims=True) + jnp.sum(x1 * x1, axis=1, keepdims=True)
    ) / total
    inv = lax.rsqrt(spread + LN_EPS)
    n0 = (x0 * inv * gain[:, :width] + bias[:, :width]).astype(BF)
    n1 = (x1 * inv * gain[:, width:] + bias[:, width:]).astype(BF)
    return n0, n1


def kernel(
    cfg, res, q, k, v, off, wout, gain, bias, routing, rw, wg, wu, wd, sg, su, sd, out,
    wout_v, wg_v, wu_v, wd_v, sg_v, su_v, sd_v,
    kbuf, vbuf, acc, beyond, pj, r1, ys1, yr1, mixh, resall, rall, rwall,
    tok, outg, xb, yb, rb, ry, zb, ret, spart, rs, rsy, fin,
    wsem, ksend, krecv, vsend, vrecv, dsend, drecv, ysend, yrecv, asend, arecv,
    bsend, brecv, y3send, y3recv, zsend, zrecv, msend, mrecv, fksend, fvsend,
):
    n, cap2, rows, span = cfg
    i, t = lax.axis_index("sp"), lax.axis_index("tp")
    c, y = lax.rem(t, 2), lax.div(t, 2)
    oc, oy = 1 - c, 1 - y
    mate, across = t + 1 - 2 * c, t + 2 - 4 * y
    shard = q.shape[0]
    half = out.shape[1] // 2
    pair = 2 * rows

    weights = [
        pltpu.make_async_copy(src, dst, wsem.at[a])
        for a, (src, dst) in enumerate(
            [(wout, wout_v), (sg, sg_v), (su, su_v), (sd, sd_v),
             (wg.at[0], wg_v), (wu.at[0], wu_v), (wd.at[0], wd_v)]
        )
    ]
    for cp in weights:
        cp.start()

    barrier = pltpu.get_barrier_semaphore()

    def hello(d, _):
        pl.semaphore_signal(
            barrier, inc=1, device_id={"sp": lax.rem(i + d, n), "tp": t}, device_id_type=MESH
        )
        return 0

    lax.fori_loop(1, n, hello, 0)
    for peer in (mate, across):
        pl.semaphore_signal(barrier, inc=1, device_id={"sp": i, "tp": peer}, device_id_type=MESH)

    def rcopy(src, dst, ssem, rsem, sp, tp):
        return pltpu.make_async_remote_copy(
            src_ref=src, dst_ref=dst, send_sem=ssem, recv_sem=rsem,
            device_id={"sp": sp, "tp": tp}, device_id_type=MESH,
        )

    def small(m, src, dst, peer):
        return rcopy(src, dst, msend.at[m], mrecv.at[m], i, peer)

    def kcopy(dest, slot):
        return rcopy(k, kbuf.at[slot], ksend.at[dest], krecv.at[slot], dest, t)

    def vcopy(dest, slot):
        return rcopy(v, vbuf.at[slot], vsend.at[dest], vrecv.at[slot], dest, t)

    layer, lane = lax.div(i, span), lax.rem(i, span)

    def forward_kv(slot, peer):
        dest = layer * span + peer
        kc = rcopy(kbuf.at[slot], kbuf.at[slot],
                   fksend.at[slot, peer], krecv.at[slot], dest, t)
        vc = rcopy(vbuf.at[slot], vbuf.at[slot],
                   fvsend.at[slot, peer], vrecv.at[slot], dest, t)
        return kc, vc

    def push_lane(d, _):
        kcopy(i + d, i).start()
        vcopy(i + d, i).start()
        return 0

    def push_layer(d, _):
        dest = (n // span - d) * span + lane
        kcopy(dest, i).start()
        vcopy(dest, i).start()
        return 0

    def push_all():
        lax.fori_loop(1, span - lane, push_lane, 0)
        lax.fori_loop(1, n // span - layer, push_layer, 0)

    m_res = small(0, res, resall.at[c], mate)
    m_rou = small(1, routing, rall.at[c], mate)
    m_rw = small(2, rw, rwall.at[c], mate)
    resall[c] = res[...]
    rall[c] = routing[...]
    rwall[c] = rw[...]

    heads = q.shape[1] // DH
    hq = heads * shard
    q2 = jnp.concatenate([q[:, h * DH:(h + 1) * DH] for h in range(heads)], axis=0)
    row = lax.broadcasted_iota(jnp.int32, (hq, shard), 0)
    col = lax.broadcasted_iota(jnp.int32, (hq, shard), 1)
    offs = jnp.full((hq, shard), off[0], F32)
    for h in range(1, heads):
        offs = jnp.where(row >= h * shard, off[h], offs)
    trow = lax.broadcasted_iota(jnp.int32, (shard, shard), 0)
    tcol = lax.broadcasted_iota(jnp.int32, (shard, shard), 1)
    later = jnp.where(trow > tcol, 1.0, 0.0).astype(BF)
    scale = DH**-0.5

    def stick(kb, vb, causal, prior):
        s = lax.dot_general(q2, kb, (((1,), (1,)), ((), ())), preferred_element_type=F32)
        s = s * scale + offs
        soft = jnp.maximum(s, 0.0) + jnp.log(1.0 + jnp.exp(-jnp.abs(s)))
        left = -soft if causal is None else jnp.where(causal, -soft, 0.0)
        hi = left.astype(BF)
        lo = (left - hi.astype(F32)).astype(BF)
        within = dot(hi, later) + dot(lo, later)
        w = jnp.exp(s - soft + within + prior)
        if causal is not None:
            w = jnp.where(causal, w, 0.0)
        total = jnp.sum(left, axis=1, keepdims=True)
        return dot(w.astype(BF), vb), total

    o, total = stick(k[...], v[...], col < lax.rem(row, shard), 0.0)
    acc[...] = o
    beyond[...] = jnp.broadcast_to(total, (hq, shard))

    pl.semaphore_wait(barrier, n + 1)
    push_all()
    for cp in (m_res, m_rou, m_rw):
        cp.start()

    def block(src):
        o, total = stick(kbuf[src], vbuf[src], None, beyond[...])
        acc[...] += o
        beyond[...] += total

    def arrive(src):
        kcopy(i, src).wait_recv()
        vcopy(i, src).wait_recv()

    def own_layer(d, _):
        arrive(i - d)
        block(i - d)
        return 0

    lax.fori_loop(1, lane + 1, own_layer, 0)

    def earlier_layer(d, _):
        first = (layer - d) * span
        direct = first + lane
        arrive(direct)

        def hand_on(p, _):
            for cp in forward_kv(direct, lax.rem(lane + p, span)):
                cp.start()
            return 0

        lax.fori_loop(1, span, hand_on, 0)

        def one(p, _):
            src = first + span - 1 - p

            @pl.when(src != direct)
            def _():
                arrive(src)

            block(src)
            return 0

        lax.fori_loop(0, span, one, 0)
        return 0

    lax.fori_loop(1, layer + 1, earlier_layer, 0)
    att = jnp.concatenate(
        [acc[h * shard:(h + 1) * shard, :] for h in range(heads)], axis=1
    ).astype(BF)

    weights[0].wait()

    def project(h):
        columns = pl.ds(pl.multiple_of(h * half, half), half)
        pj[h] = dot(att, wout_v[:, columns]).astype(BF)

    project(oc)
    m_pj = small(3, pj.at[oc], r1, mate)
    m_pj.start()
    project(c)
    m_pj.wait_recv()
    mine_rows = pl.ds(pl.multiple_of(y * pair, pair), pair)
    other_rows = pl.ds(pl.multiple_of(oy * pair, pair), pair)
    ys1[...] = (pj[c, other_rows, :].astype(F32) + r1[other_rows, :].astype(F32)).astype(BF)
    m_y1 = small(4, ys1, yr1, across)
    m_y1.start()

    m_rou.wait_recv()
    m_rw.wait_recv()
    width = n * cap2
    rt = jnp.concatenate([rall[0], rall[1]], axis=1)
    wt = jnp.concatenate([rwall[0], rwall[1]], axis=1)
    wrow = lax.broadcasted_iota(jnp.int32, (width, pair), 0)
    e_of = lax.div(wrow, cap2)
    r_of = wrow - e_of * cap2
    is0, is1 = rt[0:1, :] == e_of, rt[1:2, :] == e_of
    named = jnp.where(is0 | is1, 1.0, 0.0)
    before = jnp.where(
        lax.broadcasted_iota(jnp.int32, (pair, pair), 0)
        < lax.broadcasted_iota(jnp.int32, (pair, pair), 1), 1.0, 0.0
    ).astype(BF)
    rank = dot(named.astype(BF), before)
    place = jnp.where(rank == r_of.astype(F32), named, 0.0)
    back = (place * jnp.where(is0, wt[0:1, :], wt[1:2, :])).T
    place_t = place.astype(BF)

    m_y1.wait_recv()
    mixh[c] = (
        pj[c, mine_rows, :].astype(F32) + r1[mine_rows, :].astype(F32) + yr1[...].astype(F32)
    )
    m_mix = small(5, mixh.at[c], mixh.at[c], mate)
    m_mix.start()
    m_res.wait_recv()
    small(5, mixh.at[oc], mixh.at[oc], mate).wait_recv()
    resid = jnp.concatenate([resall[0], resall[1]], axis=0)
    n0, n1 = layer_norm(
        ALPHA * resid[:, :half].astype(F32) + mixh[0],
        ALPHA * resid[:, half:].astype(F32) + mixh[1],
        gain[0:1, :], bias[0:1, :],
    )
    tok[y, 0] = n0
    tok[y, 1] = n1
    m_tok = small(6, tok.at[y, c], tok.at[y, c], across)
    m_tok.start()

    chosen = dot(place_t, tok[y, c])
    for e in range(n):
        outg[e] = chosen[e * cap2:(e + 1) * cap2, :].astype(BF)

    def dcopy(dest, slot):
        return rcopy(
            outg.at[dest], xb.at[c, y, slot], dsend.at[dest], drecv.at[slot], dest, t
        )

    def send_out(d, _):
        dcopy(lax.rem(i + d, n), i).start()
        return 0

    lax.fori_loop(1, n, send_out, 0)
    xb[c, y, i] = outg[i]

    def ycopy(slot, yy):
        ref = xb.at[c, yy, slot]
        return rcopy(ref, ref, ysend.at[slot], yrecv.at[slot], i, across)

    def acopy(slot, cc):
        ref = xb.at[cc, y, slot]
        return rcopy(ref, ref, asend.at[slot], arecv.at[slot], i, mate)

    def bcopy(slot, cc):
        ref = xb.at[cc, oy, slot]
        return rcopy(ref, ref, bsend.at[slot], brecv.at[slot], i, mate)

    def forward(slot):
        ycopy(slot, y).start()
        acopy(slot, c).start()

    forward(i)
    small(6, tok.at[oy, c], tok.at[oy, c], across).wait_recv()
    m_tok2 = small(7, tok.at[oy, c], tok.at[oy, c], mate)
    m_tok2.start()

    def relay(d, _):
        src = lax.rem(i + n - d, n)
        dcopy(i, src).wait_recv()
        forward(src)
        return 0

    early = n // 2
    lax.fori_loop(1, early, relay, 0)

    small(7, tok.at[oy, oc], tok.at[oy, oc], mate).wait_recv()
    for cp in weights[1:4]:
        cp.wait()
    t0 = jnp.concatenate([tok[0, 0], tok[1, 0]], axis=0)
    t1 = jnp.concatenate([tok[0, 1], tok[1, 1]], axis=0)
    gate = dot(t0, sg_v[:half, :]) + dot(t1, sg_v[half:, :])
    up = dot(t0, su_v[:half, :]) + dot(t1, su_v[half:, :])
    hid = silu_mul(gate, up)
    for h in range(2):
        spart[h] = dot(hid, sd_v[:, h * half:(h + 1) * half]).astype(BF)
    m_sp = small(8, spart.at[oc], rs, mate)
    m_sp.start()
    lax.fori_loop(early, n, relay, 0)

    def relay2(d, _):
        src = lax.rem(i + n - d, n)
        ycopy(src, oy).wait_recv()
        bcopy(src, c).start()
        return 0

    lax.fori_loop(0, early, relay2, 0)

    def gathered_own(d, _):
        acopy(lax.rem(i + n - d, n), oc).wait_recv()
        return 0

    lax.fori_loop(0, n, gathered_own, 0)
    for cp in weights[4:]:
        cp.wait()

    def expert(yy):
        x0 = xb[0, yy].astype(F32).reshape(n * cap2, half).astype(BF)
        x1 = xb[1, yy].astype(F32).reshape(n * cap2, half).astype(BF)
        gate = dot(x0, wg_v[:half, :]) + dot(x1, wg_v[half:, :])
        up = dot(x0, wu_v[:half, :]) + dot(x1, wu_v[half:, :])
        return silu_mul(gate, up)

    def down(hid, yy, h):
        columns = pl.ds(pl.multiple_of(h * half, half), half)
        yb[h, yy] = dot(hid, wd_v[:, columns]).reshape(n, cap2, half).astype(BF)

    hid = expert(y)
    down(hid, y, oc)
    m_yb1 = small(11, yb.at[oc, y], rb.at[y], mate)
    m_yb1.start()
    down(hid, y, c)
    lax.fori_loop(early, n, relay2, 0)
    m_sp.wait_recv()
    spart[c, other_rows, :] = (
        spart[c, other_rows, :].astype(F32) + rs[other_rows, :].astype(F32)
    ).astype(BF)
    m_sy = small(9, spart.at[c, other_rows, :], rsy, across)
    m_sy.start()

    def gathered(d, _):
        bcopy(lax.rem(i + n - d, n), oc).wait_recv()
        return 0

    lax.fori_loop(0, n, gathered, 0)
    hid = expert(oy)
    down(hid, oy, oc)
    m_yb0 = small(10, yb.at[oc, oy], rb.at[oy], mate)
    m_yb0.start()
    down(hid, oy, c)

    def y3copy(slot):
        return rcopy(
            yb.at[c, oy, slot], ry.at[slot], y3send.at[slot], y3recv.at[slot], i, across
        )

    def zcopy(dest, slot):
        return rcopy(zb.at[dest], ret.at[slot], zsend.at[dest], zrecv.at[slot], dest, t)

    small(10, yb.at[oc, oy], rb.at[oy], mate).wait_recv()

    def fold(d, _):
        j = lax.rem(i + d, n)
        yb[c, oy, j] = (yb[c, oy, j].astype(F32) + rb[oy, j].astype(F32)).astype(BF)
        y3copy(j).start()
        return 0

    lax.fori_loop(1, n + 1, fold, 0)
    small(11, yb.at[oc, y], rb.at[y], mate).wait_recv()

    def fold2(d, _):
        j = lax.rem(i + d, n)
        y3copy(j).wait_recv()
        zb[j] = (
            yb[c, y, j].astype(F32) + rb[y, j].astype(F32) + ry[j].astype(F32)
        ).astype(BF)
        zcopy(j, i).start()
        return 0

    lax.fori_loop(1, n, fold2, 0)
    y3copy(i).wait_recv()
    ret[i] = (yb[c, y, i].astype(F32) + rb[y, i].astype(F32) + ry[i].astype(F32)).astype(BF)

    m_sy.wait_recv()
    shared = (
        spart[c, mine_rows, :].astype(F32) + rs[mine_rows, :].astype(F32) + rsy[...].astype(F32)
    ).astype(BF).astype(F32)
    b_hi = back.astype(BF)
    b_lo = (back - b_hi.astype(F32)).astype(BF)

    def returned(d, _):
        zcopy(i, lax.rem(i + n - d, n)).wait_recv()
        return 0

    lax.fori_loop(1, n, returned, 0)
    rows_back = ret[...].astype(F32).reshape(width, half).astype(BF)
    m_mix.wait_send()
    mixh[0] = shared + dot(b_hi, rows_back) + dot(b_lo, rows_back)
    own = pl.ds(pl.multiple_of(c * rows, rows), rows)
    theirs = pl.ds(pl.multiple_of(oc * rows, rows), rows)
    fin[2] = mixh[0, theirs, :]
    fin[c] = mixh[0, own, :]
    m_fin = small(12, fin.at[2], fin.at[c], mate)
    m_fin.start()
    small(12, fin.at[2], fin.at[oc], mate).wait_recv()
    n0, n1 = layer_norm(
        ALPHA * tok[y, 0, own, :].astype(F32) + fin[0],
        ALPHA * tok[y, 1, own, :].astype(F32) + fin[1],
        gain[1:2, :], bias[1:2, :],
    )
    out[:, :half] = n0
    out[:, half:] = n1

    def sent_lane(d, _):
        kcopy(i + d, i).wait_send()
        vcopy(i + d, i).wait_send()
        return 0

    def sent_layer(d, _):
        dest = (n // span - d) * span + lane
        kcopy(dest, i).wait_send()
        vcopy(dest, i).wait_send()
        return 0

    def sent_on(d, _):
        def to_peer(p, _):
            for cp in forward_kv((layer - d) * span + lane, lax.rem(lane + p, span)):
                cp.wait_send()
            return 0

        lax.fori_loop(1, span, to_peer, 0)
        return 0

    lax.fori_loop(1, span - lane, sent_lane, 0)
    lax.fori_loop(1, n // span - layer, sent_layer, 0)
    lax.fori_loop(1, layer + 1, sent_on, 0)

    def sent(d, _):
        j = lax.rem(i + d, n)
        dcopy(j, i).wait_send()
        zcopy(j, i).wait_send()
        return 0

    lax.fori_loop(1, n, sent, 0)

    def sent_all(j, _):
        ycopy(j, y).wait_send()
        acopy(j, c).wait_send()
        bcopy(j, c).wait_send()
        y3copy(j).wait_send()
        return 0

    lax.fori_loop(0, n, sent_all, 0)
    for cp in (m_res, m_rou, m_rw, m_pj, m_y1, m_tok, m_tok2, m_sp, m_sy, m_yb0, m_yb1, m_fin):
        cp.wait_send()


def per_device(
    residual, query_rows, key_rows, value_rows, head_offset, w_out, norm_gain, norm_bias,
    routing, route_weight, w_exp_gate, w_exp_up, w_exp_down, w_shared_gate, w_shared_up,
    w_shared_down,
):
    n = lax.axis_size("sp")
    rows, width = residual.shape
    shard = query_rows.shape[0]
    half = width // 2
    heads = query_rows.shape[1] // DH
    ff = w_exp_gate.shape[2]
    sff = w_shared_gate.shape[1]
    pair = 2 * rows
    experts = n * w_exp_gate.shape[0]
    assert w_exp_gate.shape[0] == 1 and key_rows.shape[1] == DH and lax.axis_size("tp") == 4
    cap = max(2, 3 * rows * routing.shape[1] // (2 * experts))
    cap2 = -(-2 * cap // 8) * 8
    span = max(s for s in range(1, n + 1) if n % s == 0 and s * s <= n)
    vm = pl.BlockSpec(memory_space=pltpu.VMEM)
    anyw = pl.BlockSpec(memory_space=pl.ANY)
    smem = pl.BlockSpec(memory_space=pltpu.SMEM)
    dma = pltpu.SemaphoreType.DMA
    V = pltpu.VMEM
    scratch = [
        V(w_out.shape, BF), V(w_exp_gate.shape[1:], BF), V(w_exp_up.shape[1:], BF),
        V(w_exp_down.shape[1:], BF), V(w_shared_gate.shape, BF), V(w_shared_up.shape, BF),
        V(w_shared_down.shape, BF),
        V((n, shard, DH), BF), V((n, shard, DH), BF),
        V((heads * shard, DH), F32), V((heads * shard, shard), F32),
        V((2, shard, half), BF), V((shard, half), BF),
        V((pair, half), BF), V((pair, half), BF),
        V((2, pair, half), F32), V((2, rows, width), BF),
        V((2,) + routing.shape[::-1], jnp.int32), V((2,) + route_weight.shape[::-1], F32),
        V((2, 2, pair, half), BF),
        V((n, cap2, half), BF),
        V((2, 2, n, cap2, half), BF),
        V((2, 2, n, cap2, half), BF),
        V((2, n, cap2, half), BF),
        V((n, cap2, half), BF), V((n, cap2, half), BF), V((n, cap2, half), BF),
        V((2, shard, half), BF), V((shard, half), BF), V((pair, half), BF),
        V((3, rows, half), F32),
        dma((7,)),
    ] + [dma((n,))] * 16 + [dma((13,)), dma((13,)), dma((n, span)), dma((n, span))]
    return pl.pallas_call(
        functools.partial(kernel, (n, cap2, rows, span)),
        out_shape=jax.ShapeDtypeStruct(residual.shape, BF),
        in_specs=[vm, vm, vm, vm, smem, anyw, vm, vm, vm, vm] + [anyw] * 6,
        out_specs=vm,
        scratch_shapes=scratch,
        compiler_params=pltpu.CompilerParams(
            collective_id=0, has_side_effects=True, vmem_limit_bytes=56 * 1024 * 1024
        ),
    )(
        residual, query_rows, key_rows, value_rows, head_offset, w_out, norm_gain, norm_bias,
        routing.T, route_weight.T, w_exp_gate, w_exp_up, w_exp_down, w_shared_gate,
        w_shared_up, w_shared_down,
    )


def solution(mesh):
    placed = (
        P(("sp", "tp"), None),
        P("sp", "tp"),
        P("sp", "tp"),
        P("sp", "tp"),
        P("tp"),
        P("tp", None),
        P(),
        P(),
        P(("sp", "tp"), None),
        P(("sp", "tp"), None),
        P("sp", None, "tp"),
        P("sp", None, "tp"),
        P("sp", "tp", None),
        P(None, "tp"),
        P(None, "tp"),
        P("tp", None),
    )
    return jax.shard_map(
        per_device, mesh=mesh, in_specs=placed, out_specs=P(("sp", "tp"), None), check_vma=False
    )
```

```python
import functools

import jax
import jax.numpy as jnp
from jax import lax
from jax.experimental import pallas as pl
from jax.experimental.pallas import tpu as pltpu
from jax.sharding import PartitionSpec as P

DH = 128
ALPHA = 8.0**0.25
LN_EPS = 1e-05
BF = jnp.bfloat16
F32 = jnp.float32
MESH = pl.DeviceIdType.MESH


def dot(a, b):
    return jnp.dot(a, b, preferred_element_type=F32)


def silu_mul(g, u):
    return (g / (1.0 + jnp.exp(-g)) * u).astype(BF)


def layer_norm(x0, x1, gain, bias):
    width = x0.shape[1]
    total = 2 * width
    mean = (jnp.sum(x0, axis=1, keepdims=True) + jnp.sum(x1, axis=1, keepdims=True)) / total
    x0, x1 = x0 - mean, x1 - mean
    spread = (
        jnp.sum(x0 * x0, axis=1, keepdims=True) + jnp.sum(x1 * x1, axis=1, keepdims=True)
    ) / total
    inv = lax.rsqrt(spread + LN_EPS)
    n0 = (x0 * inv * gain[:, :width] + bias[:, :width]).astype(BF)
    n1 = (x1 * inv * gain[:, width:] + bias[:, width:]).astype(BF)
    return n0, n1


def kernel(
    cfg, res, q, k, v, off, wout, gain, bias, routing, rw, wg, wu, wd, sg, su, sd, out,
    wout_v, wg_v, wu_v, wd_v, sg_v, su_v, sd_v,
    kbuf, vbuf, acc, beyond, pj, r1, ys1, yr1, mixh, resall, rall, rwall,
    tok, outg, xb, yb, rb, ry, zb, ret, spart, rs, rsy, fin,
    wsem, ksend, krecv, vsend, vrecv, dsend, drecv, ysend, yrecv, asend, arecv,
    bsend, brecv, y3send, y3recv, zsend, zrecv, msend, mrecv, fksend, fvsend,
    y0send, y0recv, comb,
):
    n, cap2, rows, span = cfg
    i, t = lax.axis_index("sp"), lax.axis_index("tp")
    c, y = lax.rem(t, 2), lax.div(t, 2)
    oc, oy = 1 - c, 1 - y
    mate, across = t + 1 - 2 * c, t + 2 - 4 * y
    shard = q.shape[0]
    half = out.shape[1] // 2
    pair = 2 * rows

    weights = [
        pltpu.make_async_copy(src, dst, wsem.at[a])
        for a, (src, dst) in enumerate(
            [(wout, wout_v), (sg, sg_v), (su, su_v), (sd, sd_v),
             (wg.at[0], wg_v), (wu.at[0], wu_v), (wd.at[0], wd_v)]
        )
    ]
    for cp in weights:
        cp.start()

    barrier = pltpu.get_barrier_semaphore()

    def hello(d, _):
        pl.semaphore_signal(
            barrier, inc=1, device_id={"sp": lax.rem(i + d, n), "tp": t}, device_id_type=MESH
        )
        return 0

    lax.fori_loop(1, n, hello, 0)
    for peer in (mate, across):
        pl.semaphore_signal(barrier, inc=1, device_id={"sp": i, "tp": peer}, device_id_type=MESH)

    def rcopy(src, dst, ssem, rsem, sp, tp):
        return pltpu.make_async_remote_copy(
            src_ref=src, dst_ref=dst, send_sem=ssem, recv_sem=rsem,
            device_id={"sp": sp, "tp": tp}, device_id_type=MESH,
        )

    def small(m, src, dst, peer):
        return rcopy(src, dst, msend.at[m], mrecv.at[m], i, peer)

    def kcopy(dest, slot):
        return rcopy(k, kbuf.at[slot], ksend.at[dest], krecv.at[slot], dest, t)

    def vcopy(dest, slot):
        return rcopy(v, vbuf.at[slot], vsend.at[dest], vrecv.at[slot], dest, t)

    layer, lane = lax.div(i, span), lax.rem(i, span)

    def forward_kv(slot, peer):
        dest = layer * span + peer
        kc = rcopy(kbuf.at[slot], kbuf.at[slot],
                   fksend.at[slot, peer], krecv.at[slot], dest, t)
        vc = rcopy(vbuf.at[slot], vbuf.at[slot],
                   fvsend.at[slot, peer], vrecv.at[slot], dest, t)
        return kc, vc

    def push_lane(d, _):
        kcopy(i + d, i).start()
        vcopy(i + d, i).start()
        return 0

    def push_layer(d, _):
        dest = (n // span - d) * span + lane
        kcopy(dest, i).start()
        vcopy(dest, i).start()
        return 0

    def push_all():
        lax.fori_loop(1, span - lane, push_lane, 0)
        lax.fori_loop(1, n // span - layer, push_layer, 0)

    m_res = small(0, res, resall.at[c], mate)
    m_rou = small(1, routing, rall.at[c], mate)
    m_rw = small(2, rw, rwall.at[c], mate)
    resall[c] = res[...]
    rall[c] = routing[...]
    rwall[c] = rw[...]

    heads = q.shape[1] // DH
    hq = heads * shard
    q2 = jnp.concatenate([q[:, h * DH:(h + 1) * DH] for h in range(heads)], axis=0)
    row = lax.broadcasted_iota(jnp.int32, (hq, shard), 0)
    col = lax.broadcasted_iota(jnp.int32, (hq, shard), 1)
    offs = jnp.full((hq, shard), off[0], F32)
    for h in range(1, heads):
        offs = jnp.where(row >= h * shard, off[h], offs)
    trow = lax.broadcasted_iota(jnp.int32, (shard, shard), 0)
    tcol = lax.broadcasted_iota(jnp.int32, (shard, shard), 1)
    later = jnp.where(trow > tcol, 1.0, 0.0).astype(BF)
    scale = DH**-0.5

    def stick(kb, vb, causal, prior):
        s = lax.dot_general(q2, kb, (((1,), (1,)), ((), ())), preferred_element_type=F32)
        s = s * scale + offs
        soft = jnp.maximum(s, 0.0) + jnp.log(1.0 + jnp.exp(-jnp.abs(s)))
        left = -soft if causal is None else jnp.where(causal, -soft, 0.0)
        hi = left.astype(BF)
        lo = (left - hi.astype(F32)).astype(BF)
        within = dot(hi, later) + dot(lo, later)
        w = jnp.exp(s - soft + within + prior)
        if causal is not None:
            w = jnp.where(causal, w, 0.0)
        total = jnp.sum(left, axis=1, keepdims=True)
        return dot(w.astype(BF), vb), total

    o, total = stick(k[...], v[...], col < lax.rem(row, shard), 0.0)
    acc[...] = o
    beyond[...] = jnp.broadcast_to(total, (hq, shard))

    pl.semaphore_wait(barrier, n + 1)
    push_all()
    for cp in (m_res, m_rou, m_rw):
        cp.start()

    def block(src):
        o, total = stick(kbuf[src], vbuf[src], None, beyond[...])
        acc[...] += o
        beyond[...] += total

    def arrive(src):
        kcopy(i, src).wait_recv()
        vcopy(i, src).wait_recv()

    def own_layer(d, _):
        arrive(i - d)
        block(i - d)
        return 0

    lax.fori_loop(1, lane + 1, own_layer, 0)

    def earlier_layer(d, _):
        first = (layer - d) * span
        direct = first + lane
        arrive(direct)

        def hand_on(p, _):
            for cp in forward_kv(direct, lax.rem(lane + p, span)):
                cp.start()
            return 0

        lax.fori_loop(1, span, hand_on, 0)

        def one(p, _):
            src = first + span - 1 - p

            @pl.when(src != direct)
            def _():
                arrive(src)

            block(src)
            return 0

        lax.fori_loop(0, span, one, 0)
        return 0

    lax.fori_loop(1, layer + 1, earlier_layer, 0)
    att = jnp.concatenate(
        [acc[h * shard:(h + 1) * shard, :] for h in range(heads)], axis=1
    ).astype(BF)

    weights[0].wait()

    def project(h):
        columns = pl.ds(pl.multiple_of(h * half, half), half)
        pj[h] = dot(att, wout_v[:, columns]).astype(BF)

    mine_rows = pl.ds(pl.multiple_of(y * pair, pair), pair)
    other_rows = pl.ds(pl.multiple_of(oy * pair, pair), pair)
    project(oc)
    m_pj = small(3, pj.at[oc, other_rows, :], r1.at[other_rows, :], mate)
    m_pj2 = small(13, pj.at[oc, mine_rows, :], r1.at[mine_rows, :], mate)
    m_pj.start()
    m_pj2.start()
    project(c)
    m_pj.wait_recv()
    ys1[...] = (pj[c, other_rows, :].astype(F32) + r1[other_rows, :].astype(F32)).astype(BF)
    m_y1 = small(4, ys1, yr1, across)
    m_y1.start()

    m_rou.wait_recv()
    m_rw.wait_recv()
    width = n * cap2
    rt = jnp.concatenate([rall[0], rall[1]], axis=1)
    wt = jnp.concatenate([rwall[0], rwall[1]], axis=1)
    wrow = lax.broadcasted_iota(jnp.int32, (width, pair), 0)
    e_of = lax.div(wrow, cap2)
    r_of = wrow - e_of * cap2
    is0, is1 = rt[0:1, :] == e_of, rt[1:2, :] == e_of
    named = jnp.where(is0 | is1, 1.0, 0.0)
    before = jnp.where(
        lax.broadcasted_iota(jnp.int32, (pair, pair), 0)
        < lax.broadcasted_iota(jnp.int32, (pair, pair), 1), 1.0, 0.0
    ).astype(BF)
    rank = dot(named.astype(BF), before)
    place = jnp.where(rank == r_of.astype(F32), named, 0.0)
    back = (place * jnp.where(is0, wt[0:1, :], wt[1:2, :])).T
    place_t = place.astype(BF)

    m_pj2.wait_recv()
    m_y1.wait_recv()
    mixh[c] = (
        pj[c, mine_rows, :].astype(F32) + r1[mine_rows, :].astype(F32) + yr1[...].astype(F32)
    ).astype(BF)
    m_mix = small(5, mixh.at[c], mixh.at[c], mate)
    m_mix.start()
    m_res.wait_recv()
    small(5, mixh.at[oc], mixh.at[oc], mate).wait_recv()
    resid = jnp.concatenate([resall[0], resall[1]], axis=0)
    n0, n1 = layer_norm(
        ALPHA * resid[:, :half].astype(F32) + mixh[0].astype(F32),
        ALPHA * resid[:, half:].astype(F32) + mixh[1].astype(F32),
        gain[0:1, :], bias[0:1, :],
    )
    tok[y, 0] = n0
    tok[y, 1] = n1
    m_tok = small(6, tok.at[y, c], tok.at[y, c], across)
    m_tok.start()

    chosen = dot(place_t, tok[y, c])
    for e in range(n):
        outg[e] = chosen[e * cap2:(e + 1) * cap2, :].astype(BF)

    def dcopy(dest, slot):
        return rcopy(
            outg.at[dest], xb.at[c, y, slot], dsend.at[dest], drecv.at[slot], dest, t
        )

    def send_out(d, _):
        dcopy(lax.rem(i + d, n), i).start()
        return 0

    lax.fori_loop(1, n, send_out, 0)
    xb[c, y, i] = outg[i]

    def ycopy(slot, yy):
        ref = xb.at[c, yy, slot]
        return rcopy(ref, ref, ysend.at[slot], yrecv.at[slot], i, across)

    def acopy(slot, cc):
        ref = xb.at[cc, y, slot]
        return rcopy(ref, ref, asend.at[slot], arecv.at[slot], i, mate)

    def bcopy(slot, cc):
        ref = xb.at[cc, oy, slot]
        return rcopy(ref, ref, bsend.at[slot], brecv.at[slot], i, mate)

    def forward(slot):
        ycopy(slot, y).start()
        acopy(slot, c).start()

    forward(i)
    small(6, tok.at[oy, c], tok.at[oy, c], across).wait_recv()
    m_tok2 = small(7, tok.at[oy, c], tok.at[oy, c], mate)
    m_tok2.start()

    def relay(d, _):
        src = lax.rem(i + n - d, n)
        dcopy(i, src).wait_recv()
        forward(src)
        return 0

    early = n // 2
    lax.fori_loop(1, early, relay, 0)

    small(7, tok.at[oy, oc], tok.at[oy, oc], mate).wait_recv()
    for cp in weights[1:4]:
        cp.wait()
    t0 = jnp.concatenate([tok[0, 0], tok[1, 0]], axis=0)
    t1 = jnp.concatenate([tok[0, 1], tok[1, 1]], axis=0)
    gate = dot(t0, sg_v[:half, :]) + dot(t1, sg_v[half:, :])
    up = dot(t0, su_v[:half, :]) + dot(t1, su_v[half:, :])
    hid = silu_mul(gate, up)
    for h in range(2):
        spart[h] = dot(hid, sd_v[:, h * half:(h + 1) * half]).astype(BF)
    m_sp = small(8, spart.at[oc], rs, mate)
    m_sp.start()
    lax.fori_loop(early, n, relay, 0)

    def relay2(d, _):
        src = lax.rem(i + n - d, n)
        ycopy(src, oy).wait_recv()
        bcopy(src, c).start()
        return 0

    lax.fori_loop(0, early, relay2, 0)

    def gathered_own(d, _):
        acopy(lax.rem(i + n - d, n), oc).wait_recv()
        return 0

    lax.fori_loop(0, n, gathered_own, 0)
    for cp in weights[4:]:
        cp.wait()

    def expert(yy):
        x0 = xb[0, yy].astype(F32).reshape(n * cap2, half).astype(BF)
        x1 = xb[1, yy].astype(F32).reshape(n * cap2, half).astype(BF)
        gate = dot(x0, wg_v[:half, :]) + dot(x1, wg_v[half:, :])
        up = dot(x0, wu_v[:half, :]) + dot(x1, wu_v[half:, :])
        return silu_mul(gate, up)

    def down(hid, yy, h):
        columns = pl.ds(pl.multiple_of(h * half, half), half)
        yb[h, yy] = dot(hid, wd_v[:, columns]).reshape(n, cap2, half).astype(BF)

    hid = expert(y)
    down(hid, y, oc)
    m_yb1 = small(11, yb.at[oc, y], rb.at[y], mate)
    m_yb1.start()
    down(hid, y, c)
    lax.fori_loop(early, n, relay2, 0)
    m_sp.wait_recv()
    spart[c, other_rows, :] = (
        spart[c, other_rows, :].astype(F32) + rs[other_rows, :].astype(F32)
    ).astype(BF)
    m_sy = small(9, spart.at[c, other_rows, :], rsy, across)
    m_sy.start()

    def gathered(d, _):
        bcopy(lax.rem(i + n - d, n), oc).wait_recv()
        return 0

    lax.fori_loop(0, n, gathered, 0)
    hid = expert(oy)
    down(hid, oy, oc)

    def y0copy(slot):
        return rcopy(
            yb.at[oc, oy, slot], rb.at[oy, slot], y0send.at[slot], y0recv.at[slot], i, mate
        )

    def swap_out(d, _):
        y0copy(lax.rem(i + d, n)).start()
        return 0

    lax.fori_loop(1, n + 1, swap_out, 0)
    down(hid, oy, c)

    def y3copy(slot):
        return rcopy(
            yb.at[c, oy, slot], ry.at[slot], y3send.at[slot], y3recv.at[slot], i, across
        )

    def zcopy(dest, slot):
        return rcopy(zb.at[dest], ret.at[slot], zsend.at[dest], zrecv.at[slot], dest, t)


    def fold(d, _):
        j = lax.rem(i + d, n)
        y0copy(j).wait_recv()
        yb[c, oy, j] = (yb[c, oy, j].astype(F32) + rb[oy, j].astype(F32)).astype(BF)
        y3copy(j).start()
        return 0

    lax.fori_loop(1, n + 1, fold, 0)
    small(11, yb.at[oc, y], rb.at[y], mate).wait_recv()

    def fold2(d, _):
        j = lax.rem(i + d, n)
        y3copy(j).wait_recv()
        zb[j] = (
            yb[c, y, j].astype(F32) + rb[y, j].astype(F32) + ry[j].astype(F32)
        ).astype(BF)
        zcopy(j, i).start()
        return 0

    lax.fori_loop(1, n, fold2, 0)
    y3copy(i).wait_recv()
    ret[i] = (yb[c, y, i].astype(F32) + rb[y, i].astype(F32) + ry[i].astype(F32)).astype(BF)

    m_sy.wait_recv()
    shared = (
        spart[c, mine_rows, :].astype(F32) + rs[mine_rows, :].astype(F32) + rsy[...].astype(F32)
    ).astype(BF).astype(F32)
    b_hi = back.astype(BF)
    b_lo = (back - b_hi.astype(F32)).astype(BF)

    def returned(d, _):
        zcopy(i, lax.rem(i + n - d, n)).wait_recv()
        return 0

    lax.fori_loop(1, n, returned, 0)
    rows_back = ret[...].astype(F32).reshape(width, half).astype(BF)
    comb[...] = shared + dot(b_hi, rows_back) + dot(b_lo, rows_back)
    own = pl.ds(pl.multiple_of(c * rows, rows), rows)
    theirs = pl.ds(pl.multiple_of(oc * rows, rows), rows)
    fin[2] = comb[theirs, :]
    fin[c] = comb[own, :]
    m_fin = small(12, fin.at[2], fin.at[c], mate)
    m_fin.start()
    small(12, fin.at[2], fin.at[oc], mate).wait_recv()
    n0, n1 = layer_norm(
        ALPHA * tok[y, 0, own, :].astype(F32) + fin[0],
        ALPHA * tok[y, 1, own, :].astype(F32) + fin[1],
        gain[1:2, :], bias[1:2, :],
    )
    out[:, :half] = n0
    out[:, half:] = n1

    def sent_lane(d, _):
        kcopy(i + d, i).wait_send()
        vcopy(i + d, i).wait_send()
        return 0

    def sent_layer(d, _):
        dest = (n // span - d) * span + lane
        kcopy(dest, i).wait_send()
        vcopy(dest, i).wait_send()
        return 0

    def sent_on(d, _):
        def to_peer(p, _):
            for cp in forward_kv((layer - d) * span + lane, lax.rem(lane + p, span)):
                cp.wait_send()
            return 0

        lax.fori_loop(1, span, to_peer, 0)
        return 0

    lax.fori_loop(1, span - lane, sent_lane, 0)
    lax.fori_loop(1, n // span - layer, sent_layer, 0)
    lax.fori_loop(1, layer + 1, sent_on, 0)

    def sent(d, _):
        j = lax.rem(i + d, n)
        dcopy(j, i).wait_send()
        zcopy(j, i).wait_send()
        return 0

    lax.fori_loop(1, n, sent, 0)

    def sent_all(j, _):
        ycopy(j, y).wait_send()
        acopy(j, c).wait_send()
        bcopy(j, c).wait_send()
        y3copy(j).wait_send()
        y0copy(j).wait_send()
        return 0

    lax.fori_loop(0, n, sent_all, 0)
    for cp in (
        m_res, m_rou, m_rw, m_pj, m_pj2, m_y1, m_mix, m_tok, m_tok2, m_sp, m_sy, m_yb1, m_fin
    ):
        cp.wait_send()


def per_device(
    residual, query_rows, key_rows, value_rows, head_offset, w_out, norm_gain, norm_bias,
    routing, route_weight, w_exp_gate, w_exp_up, w_exp_down, w_shared_gate, w_shared_up,
    w_shared_down,
):
    n = lax.axis_size("sp")
    rows, width = residual.shape
    shard = query_rows.shape[0]
    half = width // 2
    heads = query_rows.shape[1] // DH
    ff = w_exp_gate.shape[2]
    sff = w_shared_gate.shape[1]
    pair = 2 * rows
    experts = n * w_exp_gate.shape[0]
    assert w_exp_gate.shape[0] == 1 and key_rows.shape[1] == DH and lax.axis_size("tp") == 4
    cap = max(2, 3 * rows * routing.shape[1] // (2 * experts))
    cap2 = -(-2 * cap // 8) * 8
    span = max(s for s in range(1, n + 1) if n % s == 0 and s * s <= n)
    vm = pl.BlockSpec(memory_space=pltpu.VMEM)
    anyw = pl.BlockSpec(memory_space=pl.ANY)
    smem = pl.BlockSpec(memory_space=pltpu.SMEM)
    dma = pltpu.SemaphoreType.DMA
    V = pltpu.VMEM
    scratch = [
        V(w_out.shape, BF), V(w_exp_gate.shape[1:], BF), V(w_exp_up.shape[1:], BF),
        V(w_exp_down.shape[1:], BF), V(w_shared_gate.shape, BF), V(w_shared_up.shape, BF),
        V(w_shared_down.shape, BF),
        V((n, shard, DH), BF), V((n, shard, DH), BF),
        V((heads * shard, DH), F32), V((heads * shard, shard), F32),
        V((2, shard, half), BF), V((shard, half), BF),
        V((pair, half), BF), V((pair, half), BF),
        V((2, pair, half), BF), V((2, rows, width), BF),
        V((2,) + routing.shape[::-1], jnp.int32), V((2,) + route_weight.shape[::-1], F32),
        V((2, 2, pair, half), BF),
        V((n, cap2, half), BF),
        V((2, 2, n, cap2, half), BF),
        V((2, 2, n, cap2, half), BF),
        V((2, n, cap2, half), BF),
        V((n, cap2, half), BF), V((n, cap2, half), BF), V((n, cap2, half), BF),
        V((2, shard, half), BF), V((shard, half), BF), V((pair, half), BF),
        V((3, rows, half), F32),
        dma((7,)),
    ] + [dma((n,))] * 16 + [dma((14,)), dma((14,)), dma((n, span)), dma((n, span))] + [
        dma((n,)), dma((n,)), V((pair, half), F32)
    ]
    return pl.pallas_call(
        functools.partial(kernel, (n, cap2, rows, span)),
        out_shape=jax.ShapeDtypeStruct(residual.shape, BF),
        in_specs=[vm, vm, vm, vm, smem, anyw, vm, vm, vm, vm] + [anyw] * 6,
        out_specs=vm,
        scratch_shapes=scratch,
        compiler_params=pltpu.CompilerParams(
            collective_id=0, has_side_effects=True, vmem_limit_bytes=56 * 1024 * 1024
        ),
    )(
        residual, query_rows, key_rows, value_rows, head_offset, w_out, norm_gain, norm_bias,
        routing.T, route_weight.T, w_exp_gate, w_exp_up, w_exp_down, w_shared_gate,
        w_shared_up, w_shared_down,
    )


def solution(mesh):
    placed = (
        P(("sp", "tp"), None),
        P("sp", "tp"),
        P("sp", "tp"),
        P("sp", "tp"),
        P("tp"),
        P("tp", None),
        P(),
        P(),
        P(("sp", "tp"), None),
        P(("sp", "tp"), None),
        P("sp", None, "tp"),
        P("sp", None, "tp"),
        P("sp", "tp", None),
        P(None, "tp"),
        P(None, "tp"),
        P("tp", None),
    )
    return jax.shard_map(
        per_device, mesh=mesh, in_specs=placed, out_specs=P(("sp", "tp"), None), check_vma=False
    )
```
